1024 devices in a mesh: ep: 64 (over z, core), tp: 16 (over y, x).
Axes of the slice: x: 4, y: 4, z: 32, core: 2. Of those that a mesh axis runs over, the one named last changes fastest.
Arguments:
- tokens: bfloat16 [8192, 2048], P('ep'), may hold values from -6 to 6
- cotangent: bfloat16 [8192, 2048], P('ep'), may hold values from -1.796875 to 1.796875
- group_weight: float32 [8192], P('ep'), may hold values from 0.2 to 1
- expert_weight: float32 [8192, 2], P('ep'), may hold values from 0.1 to 0.9
- group_choice: int32 [8192], P('ep'), may hold values from 0 to 15, as said below
- local_choice: int32 [8192, 2], P('ep'), may hold values from 0 to 3, as said below
- w_gate: bfloat16 [64, 2048, 512], P('ep', None, 'tp'), may hold values from -0.125 to 0.125
- w_up: bfloat16 [64, 2048, 512], P('ep', None, 'tp'), may hold values from -0.125 to 0.125
- w_down: bfloat16 [64, 512, 2048], P('ep', 'tp'), may hold values from -0.25 to 0.25
Outputs:
- token_grad: float32 [8192, 2048], P('ep', 'tp')
- group_weight_grad: float32 [8192], P('ep')
- expert_weight_grad: float32 [8192, 2], P('ep')
- w_gate_grad: float32 [64, 2048, 512], P('ep', None, 'tp')
- w_up_grad: float32 [64, 2048, 512], P('ep', None, 'tp')
- w_down_grad: float32 [64, 512, 2048], P('ep', 'tp')
The draws below stay inside these ranges and needn't reach their ends.
Inputs may be any that keep to these rules, and one draw needn't show every extreme that they name: Among the 128 tokens of each device (aligned blocks of tokens), no expert 4 * group_choice + local_choice is named by more than 6 slots, and some expert is named by exactly 6 slots of every device. `local_choice`: the 2 local choices of a token differ.
All inputs are finite; a program needn't handle non-finite values.
Results may differ from the reference program's by a relative error of at most 0.006.
Values may be sent and summed in bfloat16 or wider, within the bound.
A program may use at most 64 MiB of HBM per device.

```python
import math
import jax
import jax.numpy as jnp
from jax import lax

D = 2048
F = 512
EPG = 4
TOP_K = 2
TOK_DEV = 128
TOKENS = 8192
EXPERTS = 64
GROUPS = 16
CAP = 6
N_EP = 64


def route_tables(key):
    folded = jax.random.fold_in(key, 11)
    key_hot, key_perm, key_order, key_shift, key_step = jax.random.split(folded, 5)
    block_count = TOKENS // TOK_DEV
    busiest = EPG * CAP // TOP_K
    hot_group = jax.random.randint(key_hot, (), 0, GROUPS, dtype=jnp.int32)
    arrange = jax.vmap(lambda member_key: jax.random.permutation(member_key, TOK_DEV))(jax.random.split(key_perm, block_count)).astype(jnp.int32)
    others = jax.vmap(lambda member_key: jax.random.permutation(member_key, GROUPS - 1))(jax.random.split(key_order, block_count)).astype(jnp.int32)
    places = jnp.arange(TOK_DEV, dtype=jnp.int32)
    beyond = jnp.maximum(places - busiest, 0)
    column_ids = jnp.broadcast_to(beyond % (GROUPS - 1), (block_count, TOK_DEV))
    other_pick = jnp.take_along_axis(others, column_ids, axis=1)
    other_group = other_pick + (other_pick >= hot_group).astype(jnp.int32)
    group_at = jnp.where(places[None, :] < busiest, hot_group, other_group)
    rank_at = jnp.where(places < busiest, places, beyond // (GROUPS - 1))[None, :]
    shifts = jax.random.randint(key_shift, (block_count, GROUPS), 0, EPG, dtype=jnp.int32)
    strides = jax.random.randint(key_step, (block_count, GROUPS), 1, EPG, dtype=jnp.int32)
    first_local = (rank_at + jnp.take_along_axis(shifts, group_at, axis=1)) % EPG
    stride_at = jnp.take_along_axis(strides, group_at, axis=1)
    local_at = (first_local[..., None] + jnp.arange(TOP_K, dtype=jnp.int32) * stride_at[..., None]) % EPG
    inverse = jnp.argsort(arrange, axis=1, stable=True).astype(jnp.int32)
    group_table = jnp.take_along_axis(group_at, inverse, axis=1)
    local_table = jnp.take_along_axis(local_at, inverse[..., None], axis=1)
    return (group_table.reshape(TOKENS).astype(jnp.int32), local_table.reshape(TOKENS, TOP_K).astype(jnp.int32))


def draw_group_choice(key, part):
    return route_tables(key)[0]


def draw_local_choice(key, part):
    return route_tables(key)[1]


def level_of(own_key, extent, cuts, smallest, high):
    level = 1.0
    for dim, shards_of in cuts:
        draws = jax.random.uniform(jax.random.fold_in(jax.random.fold_in(own_key, 6), dim), (shards_of,), jnp.float32, smallest / len(cuts), high / len(cuts))
        level = level * jnp.repeat(jnp.exp(draws), extent[dim] // shards_of).reshape((-1,) + (1,) * (len(extent) - 1 - dim))
    return level


def noise(own_key, dims, scale, bound, cuts=(), kind=jnp.bfloat16):
    values = jax.random.normal(own_key, dims, jnp.float32) * scale
    if len(cuts) > 0:
        values = level_of(own_key, dims, cuts, -0.22, 0.18) * values
    return jnp.clip(values, min=-bound, max=bound).astype(kind)


def setup_inputs(seed: int = 0) -> dict:
    keys = jax.random.split(jax.random.key(seed), 10)
    return {
        "tokens": noise(keys[0], (TOKENS, D), 1.0, 6.0, ((0, 64),)),
        "cotangent": noise(keys[1], (TOKENS, D), 0.3, 1.796875, ((0, 64),)),
        "group_weight": jnp.clip(jnp.exp(math.log(1.0) - 1.609438 * jax.random.uniform(keys[2], (TOKENS,), jnp.float32) ** level_of(keys[2], (TOKENS,), ((0, 64),), -0.2, 0.2)), 0.2, 1.0),
        "expert_weight": jnp.clip(0.1 + 0.79999997 * jax.random.uniform(keys[3], (TOKENS, TOP_K), jnp.float32) ** level_of(keys[3], (TOKENS, TOP_K), ((0, 64),), -0.2, 0.2), 0.1, 0.9),
        "group_choice": draw_group_choice(jax.random.fold_in(keys[9], 71), 0),
        "local_choice": draw_local_choice(jax.random.fold_in(keys[9], 71), 0),
        "w_gate": noise(keys[6], (EXPERTS, D, F), D ** -0.5, 0.125, ((0, 64), (2, 16))),
        "w_up": noise(keys[7], (EXPERTS, D, F), D ** -0.5, 0.125, ((0, 64), (2, 16))),
        "w_down": noise(keys[8], (EXPERTS, F, D), F ** -0.5, 0.25, ((0, 64), (1, 16))),
    }


def expert_backward(arrived, cot_rows, gate_rows, first, second, third):
    pre_gate = jnp.dot(arrived, first, preferred_element_type=jnp.float32)
    pre_up = jnp.dot(arrived, second, preferred_element_type=jnp.float32)
    back_hidden = jnp.dot(cot_rows, third.T, preferred_element_type=jnp.float32)
    sigma = jax.nn.sigmoid(pre_gate)
    swish = pre_gate * sigma
    hidden = swish * pre_up
    gate_part = jnp.sum(hidden * back_hidden, axis=1)
    gate_float = gate_rows.astype(jnp.float32)[:, None]
    scaled = gate_float * back_hidden
    grad_gate_pre = (scaled * pre_up * sigma * (1.0 + pre_gate * (1.0 - sigma))).astype(jnp.bfloat16)
    grad_up_pre = (scaled * swish).astype(jnp.bfloat16)
    weighted = (gate_float * hidden).astype(jnp.bfloat16)
    first_grad = jnp.dot(arrived.T, grad_gate_pre, preferred_element_type=jnp.float32)
    second_grad = jnp.dot(arrived.T, grad_up_pre, preferred_element_type=jnp.float32)
    third_grad = jnp.dot(weighted.T, cot_rows, preferred_element_type=jnp.float32)
    total = jnp.dot(grad_gate_pre, first.T, preferred_element_type=jnp.float32)
    total = total + jnp.dot(grad_up_pre, second.T, preferred_element_type=jnp.float32)
    row_grad = total.astype(jnp.bfloat16)
    return first_grad, second_grad, third_grad, row_grad, gate_part


def reference(tokens, cotangent, group_weight, expert_weight, group_choice, local_choice, w_gate, w_up, w_down):
    slot_total = TOKENS * TOP_K
    expert_of = (group_choice[:, None] * EPG + local_choice).reshape(slot_total).astype(jnp.int32)
    member = (expert_of[:, None] == jnp.arange(EXPERTS, dtype=jnp.int32)[None, :]).astype(jnp.int32)
    running = jnp.cumsum(member, axis=0).astype(jnp.int32) - 1
    position = jnp.sum(running * member, axis=1).astype(jnp.int32)
    buffer_rows = N_EP * CAP
    slot_ids = jnp.arange(slot_total, dtype=jnp.int32)
    owner = jnp.full((EXPERTS, buffer_rows), slot_total, jnp.int32).at[expert_of, position].set(slot_ids)
    gate_value = (group_weight[:, None] * expert_weight).astype(jnp.bfloat16).reshape(slot_total)

    def per_expert(index):
        chosen = owner[index]
        live = chosen < slot_total
        safe = jnp.minimum(chosen, slot_total - 1)
        token_ids = (safe // TOP_K).astype(jnp.int32)
        zero = jnp.zeros((), jnp.bfloat16)
        arrived = jnp.where(live[:, None], tokens[token_ids], zero)
        cot_rows = jnp.where(live[:, None], cotangent[token_ids], zero)
        gate_rows = jnp.where(live, gate_value[safe], zero)
        return expert_backward(arrived, cot_rows, gate_rows, w_gate[index], w_up[index], w_down[index])

    first_grad, second_grad, third_grad, row_grad, gate_part = lax.map(per_expert, jnp.arange(EXPERTS, dtype=jnp.int32))
    slot_grad = row_grad[expert_of, position].astype(jnp.float32)
    token_grad = jnp.sum(slot_grad.reshape(TOKENS, TOP_K, D), axis=1)
    held = lax.optimization_barrier(gate_part[expert_of, position].astype(jnp.bfloat16))
    gate_grad = held.astype(jnp.float32).reshape(TOKENS, TOP_K)
    group_grad = jnp.sum(expert_weight * gate_grad, axis=1)
    expert_grad = group_weight[:, None] * gate_grad
    return (token_grad, group_grad, expert_grad, first_grad, second_grad, third_grad)
```

```python
import functools

import jax
import jax.numpy as jnp
from jax import lax
from jax.experimental import pallas as pl
from jax.experimental.pallas import tpu as pltpu
from jax.sharding import Mesh
from jax.sharding import PartitionSpec as P

EPG = 4
CAP = 6
LANES = 128
MESH = pl.DeviceIdType.MESH
F32 = jnp.float32
BF16 = jnp.bfloat16
NN = (((1,), (0,)), ((), ()))
NT = (((1,), (1,)), ((), ()))
TN = (((0,), (0,)), ((), ()))


def dot(a, b, dims=NN):
    return lax.dot_general(a, b, dims, preferred_element_type=F32)


def iota(shape, dim):
    return lax.broadcasted_iota(jnp.int32, shape, dim)


def hot(mask):
    return jnp.where(mask, 1.0, 0.0).astype(BF16)


def sixth(v):
    return (v * 10923) >> 16


def body(
    nz,
    chunks,
    route_ref,
    tok_hbm,
    cot_hbm,
    wg_hbm,
    wu_hbm,
    wd_hbm,
    token_out,
    small_out,
    gate_out,
    up_out,
    down_out,
    tok_v,
    cot_v,
    w2,
    wd_in,
    wd_p,
    send,
    recv,
    gates,
    arr_t,
    arr_c,
    w_rows,
    pieces,
    parts,
    ret_send,
    ret_recv,
    load_sem,
    z_send,
    z_recv,
    w_send,
    w_recv,
    a_send,
    a_recv,
    p_send,
    p_recv,
    q_send,
    q_recv,
    r_send,
    r_recv,
):
    z, c = lax.axis_index("z"), lax.axis_index("c")
    y, x = lax.axis_index("y"), lax.axis_index("x")
    ep, j = z * 2 + c, y * 4 + x
    experts = 2 * nz
    slots = experts * CAP
    per = experts // chunks
    rows = per * CAP
    half = rows // 2

    def z_peer(i, sign):
        k = 1 + i // 2
        dz = ((k + 1) // 2) * (2 * (k % 2) - 1)
        return k, lax.rem(z + sign * dz + nz, nz), lax.rem(i, 2)

    def plane_peer(i):
        p = lax.rem(j + i, 16)
        return p, {"y": p // 4, "x": lax.rem(p, 4)}

    barrier = pltpu.get_barrier_semaphore()

    def greet_z(i, _):
        _k, zz, cc = z_peer(i, 1)
        pl.semaphore_signal(barrier, inc=1, device_id={"z": zz, "c": cc}, device_id_type=MESH)
        return 0

    def greet_plane(i, _):
        _p, where = plane_peer(i)
        pl.semaphore_signal(barrier, inc=1, device_id=where, device_id_type=MESH)
        return 0

    lax.fori_loop(0, 2 * (nz - 1), greet_z, 0)
    pl.semaphore_signal(barrier, inc=1, device_id={"c": 1 - c}, device_id_type=MESH)
    lax.fori_loop(1, 16, greet_plane, 0)

    own = pl.ds(pl.multiple_of(j * LANES, LANES), LANES)
    loads = (
        pltpu.make_async_copy(tok_hbm.at[:, own], tok_v, load_sem.at[0]),
        pltpu.make_async_copy(cot_hbm.at[:, own], cot_v, load_sem.at[1]),
        pltpu.make_async_copy(wg_hbm, w2.at[pl.ds(0, 32)], load_sem.at[2]),
        pltpu.make_async_copy(wu_hbm, w2.at[pl.ds(32, 32)], load_sem.at[3]),
        pltpu.make_async_copy(wd_hbm, wd_in, load_sem.at[4]),
    )
    for load in loads:
        load.start()

    e0, e1 = route_ref[0:1, :], route_ref[1:2, :]
    g0, g1 = route_ref[2:3, :], route_ref[3:4, :]
    group_w, ew0, ew1 = route_ref[4:5, :], route_ref[5:6, :], route_ref[6:7, :]
    count = e0.shape[1]
    before = hot(iota((count, count), 0) < iota((count, count), 1))

    def named(n_rows, shift):
        expert = (iota((n_rows, count), 0) >> shift).astype(F32)
        in0, in1 = e0 == expert, e1 == expert
        member = in0 | in1
        place = dot(hot(member), before)
        return in0, in1, member, place

    in0, in1, member, place = named(experts, 0)
    gate_of = jnp.where(in0, g0, 0.0) + jnp.where(in1, g1, 0.0)
    lane = iota((experts, LANES), 1)
    gate_block = jnp.zeros((experts, LANES), F32)
    for q in range(CAP):
        col = jnp.sum(jnp.where(member & (place == q), gate_of, 0.0), axis=1, keepdims=True)
        gate_block = jnp.where(lane == q, col, gate_block)
    _i0, _i1, member16, place16 = named(experts * 16, 4)
    within = (iota((experts * 16, count), 0) & 15).astype(F32)
    pick_t = hot(member16 & (place16 == within))
    pick_c = hot(member16 & (place16 == within - CAP))
    row_of = iota((experts * 16, experts), 0)
    pick_g = hot(
        ((row_of >> 4) == iota((experts * 16, experts), 1)) & ((row_of & 15) == 2 * CAP)
    )
    loads[0].wait()
    loads[1].wait()
    block = dot(pick_t, tok_v[...]) + dot(pick_c, cot_v[...])
    block = block + dot(pick_g, gate_block.astype(BF16))
    send[...] = block.astype(BF16).reshape(experts, 16, LANES)
    recv[pl.ds(c, 1)] = send[pl.ds(ep, 1)]
    loads[2].wait()
    loads[3].wait()
    loads[4].wait()

    pl.semaphore_wait(barrier, 2 * (nz - 1) + 1 + 15)

    def z_copy(i):
        k, zz, cc = z_peer(i, 1)
        return pltpu.make_async_remote_copy(
            src_ref=send.at[zz * 2 + cc],
            dst_ref=recv.at[2 * k + c],
            send_sem=z_send.at[2 * k + cc],
            recv_sem=z_recv.at[2 * k + c],
            device_id={"z": zz, "c": cc},
            device_id_type=MESH,
        )

    partner = pltpu.make_async_remote_copy(
        src_ref=send.at[z * 2 + 1 - c],
        dst_ref=recv.at[c],
        send_sem=z_send.at[0],
        recv_sem=z_recv.at[c],
        device_id={"c": 1 - c},
        device_id_type=MESH,
    )
    partner.start()
    lax.fori_loop(0, 2 * (nz - 1), lambda i, _: (z_copy(i).start(), 0)[1], 0)

    def w_copy(i):
        p, where = plane_peer(i)
        return pltpu.make_async_remote_copy(
            src_ref=w2.at[:, pl.ds(pl.multiple_of(p * LANES, LANES), LANES)],
            dst_ref=w_rows.at[j],
            send_sem=w_send.at[i],
            recv_sem=w_recv.at[j],
            device_id=where,
            device_id_type=MESH,
        )

    lax.fori_loop(1, 16, lambda i, _: (w_copy(i).start(), 0)[1], 0)
    w_rows[pl.ds(j, 1)] = w2[:, own].reshape(1, 64, LANES)
    for a in range(4):
        for b in range(4):
            wd_p[:, (4 * b + a) * LANES : (4 * b + a + 1) * LANES] = wd_in[
                :, (4 * a + b) * LANES : (4 * a + b + 1) * LANES
            ]

    def cols(v, u):
        return pl.ds(pl.multiple_of((4 * v + u) * LANES, LANES), LANES)

    def wide(v):
        return pl.ds(pl.multiple_of(v * 4 * LANES, 4 * LANES), 4 * LANES)

    def ring(which, chunk):
        arr, u, v, u_axis, v_axis = (
            (arr_t, x, y, "x", "y") if which == 0 else (arr_c, y, x, "y", "x")
        )
        first = chunk * rows
        full, low, high = (
            pl.ds(first, rows),
            pl.ds(first, half),
            pl.ds(first + half, half),
        )
        up, um, u2 = lax.rem(u + 1, 4), lax.rem(u + 3, 4), lax.rem(u + 2, 4)
        vp, vm, v2 = lax.rem(v + 1, 4), lax.rem(v + 3, 4), lax.rem(v + 2, 4)

        def copy(n, ref, axis, to):
            return pltpu.make_async_remote_copy(
                src_ref=ref,
                dst_ref=ref,
                send_sem=a_send.at[which, chunk, n],
                recv_sem=a_recv.at[which, chunk, n],
                device_id={axis: to},
                device_id_type=MESH,
            )

        def sent(n):
            ref = (
                arr.at[full, cols(v, u)],
                arr.at[full, cols(v, u)],
                arr.at[low, cols(v, um)],
                arr.at[high, cols(v, up)],
                arr.at[full, wide(v)],
                arr.at[full, wide(v)],
                arr.at[low, wide(vm)],
                arr.at[high, wide(vp)],
            )[n]
            to = (up, um, up, um, vp, vm, vp, vm)[n]
            return copy(n, ref, u_axis if n < 4 else v_axis, to)

        def landed(n):
            copy(
                n,
                (
                    arr.at[full, cols(v, um)],
                    arr.at[full, cols(v, up)],
                    arr.at[low, cols(v, u2)],
                    arr.at[high, cols(v, u2)],
                    arr.at[full, wide(vm)],
                    arr.at[full, wide(vp)],
                    arr.at[low, wide(v2)],
                    arr.at[high, wide(v2)],
                )[n],
                u_axis if n < 4 else v_axis,
                up if n < 4 else vp,
            ).wait_recv()

        return sent, landed

    def step(number, chunk):
        for which in range(2):
            sent, landed = ring(which, chunk)
            if number == 1:
                sent(0).start()
                sent(1).start()
            elif number == 2:
                landed(0)
                sent(2).start()
                landed(1)
                sent(3).start()
            elif number == 3:
                landed(2)
                landed(3)
                sent(4).start()
                sent(5).start()
            elif number == 4:
                landed(4)
                sent(6).start()
                landed(5)
                sent(7).start()
            else:
                landed(6)
                landed(7)

    def z_landed(slot):
        pltpu.make_async_remote_copy(
            src_ref=send.at[0],
            dst_ref=recv.at[slot],
            send_sem=z_send.at[0],
            recv_sem=z_recv.at[slot],
            device_id={"c": 1 - c},
            device_id_type=MESH,
        ).wait_recv()

    pack_rows = 2 * rows + per
    r_id, c_id = iota((pack_rows, per * 16), 0), iota((pack_rows, per * 16), 1)
    second = jnp.where(r_id >= rows, 1, 0)
    r_in = r_id - second * rows
    r_slot = sixth(r_in)
    wanted = r_slot * 16 + (r_in - r_slot * CAP) + second * CAP
    wanted = jnp.where(r_id >= 2 * rows, (r_id - 2 * rows) * 16 + 2 * CAP, wanted)
    pack = hot(c_id == wanted)

    def arrive(chunk):
        if chunk == 0:
            z_landed(1 - c)
        lax.fori_loop(
            chunk * per + (2 if chunk == 0 else 0),
            (chunk + 1) * per,
            lambda s, _: (z_landed(s), 0)[1],
            0,
        )
        got = recv[chunk * per : (chunk + 1) * per].reshape(per * 16, LANES)
        packed = dot(pack, got)
        at = pl.ds(chunk * rows, rows)
        arr_t[at, cols(y, x)] = packed[:rows].astype(BF16)
        arr_c[at, cols(x, y)] = packed[rows : 2 * rows].astype(BF16)
        gates[chunk * per : (chunk + 1) * per, :] = packed[2 * rows :]

    for chunk in range(chunks):
        arrive(chunk)
        step(1, chunk)
        if chunk:
            step(4, chunk - 1)
        step(2, chunk)
        if chunk:
            step(5, chunk - 1)
        step(3, chunk)
    step(4, chunks - 1)
    step(5, chunks - 1)

    lane_slot = sixth(iota((experts, slots), 1))
    of_slot = lane_slot == iota((experts, slots), 0)
    lane_q = iota((LANES, slots), 1)
    lane_q = lane_q - sixth(lane_q) * CAP
    spread = hot(lane_q == iota((LANES, slots), 0))
    gate_row = jnp.sum(
        jnp.where(of_slot, dot(gates[...].astype(BF16), spread), 0.0), axis=0, keepdims=True
    )
    pre = dot(w2[...], arr_t[...], NT)
    back = dot(wd_p[...], arr_c[...], NT)
    pre_gate, pre_up = pre[:32], pre[32:]
    sigma = jax.nn.sigmoid(pre_gate)
    swish = pre_gate * sigma
    hidden = swish * pre_up
    part = jnp.sum(hidden * back, axis=0, keepdims=True)
    scaled = gate_row * back
    grads = jnp.concatenate(
        [scaled * pre_up * sigma * (1.0 + pre_gate * (1.0 - sigma)), scaled * swish], axis=0
    ).astype(BF16)
    weighted = (gate_row * hidden).astype(BF16)
    pieces[pl.ds(j, 1)] = grads.reshape(1, 64, slots)
    parts[pl.ds(j, 1)] = part.reshape(1, 1, slots)

    def p_copy(i):
        _p, where = plane_peer(i)
        return pltpu.make_async_remote_copy(
            src_ref=pieces.at[j],
            dst_ref=pieces.at[j],
            send_sem=p_send.at[i],
            recv_sem=p_recv.at[j],
            device_id=where,
            device_id_type=MESH,
        )

    def q_copy(i):
        _p, where = plane_peer(i)
        return pltpu.make_async_remote_copy(
            src_ref=parts.at[j],
            dst_ref=parts.at[j],
            send_sem=q_send.at[i],
            recv_sem=q_recv.at[j],
            device_id=where,
            device_id_type=MESH,
        )

    def plane_landed(i):
        p, where = plane_peer(i)
        for ref, s_sem, r_sem in (
            (pieces, p_send, p_recv),
            (parts, q_send, q_recv),
            (w_rows, w_send, w_recv),
        ):
            pltpu.make_async_remote_copy(
                src_ref=ref.at[p],
                dst_ref=ref.at[p],
                send_sem=s_sem.at[i],
                recv_sem=r_sem.at[p],
                device_id=where,
                device_id_type=MESH,
            ).wait_recv()

    lax.fori_loop(1, 16, lambda i, _: (p_copy(i).start(), q_copy(i).start(), 0)[2], 0)
    lax.fori_loop(1, 16, lambda i, _: (plane_landed(i), 0)[1], 0)

    row_grad = dot(
        pieces[...].reshape(16 * 64, slots), w_rows[...].reshape(16 * 64, LANES), TN
    ).astype(BF16)
    total = jnp.sum(parts[...], axis=0).astype(BF16).astype(F32)
    held = dot(jnp.where(of_slot, total, 0.0).astype(BF16), spread, NT)
    r_id, c_id = iota((experts * 8, slots), 0), iota((experts * 8, slots), 1)
    unpack = hot((c_id == (r_id >> 3) * CAP + (r_id & 7)) & ((r_id & 7) < CAP))
    r_id, c_id = iota((experts * 8, experts), 0), iota((experts * 8, experts), 1)
    unheld = hot((c_id == (r_id >> 3)) & ((r_id & 7) == CAP))
    back_block = dot(unpack, row_grad) + dot(unheld, held.astype(BF16))
    ret_send[...] = back_block.astype(BF16).reshape(experts, 8, LANES)
    ret_recv[pl.ds(ep, 1)] = ret_send[pl.ds(c, 1)]

    def r_copy(i):
        k, zz, cc = z_peer(i, -1)
        return pltpu.make_async_remote_copy(
            src_ref=ret_send.at[2 * k + cc],
            dst_ref=ret_recv.at[ep],
            send_sem=r_send.at[2 * k + cc],
            recv_sem=r_recv.at[ep],
            device_id={"z": zz, "c": cc},
            device_id_type=MESH,
        )

    r_partner = pltpu.make_async_remote_copy(
        src_ref=ret_send.at[1 - c],
        dst_ref=ret_recv.at[ep],
        send_sem=r_send.at[0],
        recv_sem=r_recv.at[ep],
        device_id={"c": 1 - c},
        device_id_type=MESH,
    )
    lax.fori_loop(
        0, 2 * (nz - 1), lambda i, _: (r_copy(2 * (nz - 1) - 1 - i).start(), 0)[1], 0
    )
    r_partner.start()

    first_two = dot(grads, arr_t[...])
    gate_out[...] = first_two[:32]
    up_out[...] = first_two[32:]
    third = dot(weighted, arr_c[...])
    for a in range(4):
        for b in range(4):
            down_out[:, (4 * a + b) * LANES : (4 * a + b + 1) * LANES] = third[
                :, (4 * b + a) * LANES : (4 * b + a + 1) * LANES
            ]

    def r_landed(i):
        e = lax.rem(ep + i, experts)
        pltpu.make_async_remote_copy(
            src_ref=ret_send.at[0],
            dst_ref=ret_recv.at[e],
            send_sem=r_send.at[0],
            recv_sem=r_recv.at[e],
            device_id={"c": 1 - c},
            device_id_type=MESH,
        ).wait_recv()

    lax.fori_loop(1, experts, lambda i, _: (r_landed(i), 0)[1], 0)

    returned = ret_recv[...].reshape(experts * 8, LANES)
    _i0, _i1, member8, place8 = named(experts * 8, 3)
    within = (iota((experts * 8, count), 0) & 7).astype(F32)
    token_out[...] = dot(hot(member8 & (place8 == within)), returned, TN)
    r_id, c_id = iota((experts, experts * 8), 0), iota((experts, experts * 8), 1)
    held_back = dot(hot(c_id == r_id * 8 + CAP), returned).astype(BF16)
    held_rows = []
    for inside in (in0, in1):
        spot = jnp.sum(jnp.where(inside, place, 0.0), axis=0, keepdims=True)
        mixed = dot(held_back, hot(inside), TN)
        at_spot = iota((LANES, count), 0).astype(F32) == spot
        held_rows.append(jnp.sum(jnp.where(at_spot, mixed, 0.0), axis=0, keepdims=True))
    small_out[0:1, :] = group_w * held_rows[0]
    small_out[1:2, :] = group_w * held_rows[1]
    small_out[2:3, :] = ew0 * held_rows[0] + ew1 * held_rows[1]
    small_out[3:8, :] = jnp.zeros((5, count), F32)

    partner.wait_send()
    lax.fori_loop(0, 2 * (nz - 1), lambda i, _: (z_copy(i).wait_send(), 0)[1], 0)
    r_partner.wait_send()
    lax.fori_loop(0, 2 * (nz - 1), lambda i, _: (r_copy(i).wait_send(), 0)[1], 0)

    def plane_left(i, _):
        w_copy(i).wait_send()
        p_copy(i).wait_send()
        q_copy(i).wait_send()
        return 0

    lax.fori_loop(1, 16, plane_left, 0)
    for chunk in range(chunks):
        for which in range(2):
            sent, _landed = ring(which, chunk)
            for n in range(8):
                sent(n).wait_send()


def run(nz, chunks, route, tokens, cotangent, wg, wu, wd):
    experts = 2 * nz
    slots = experts * CAP
    count, width = tokens.shape
    dma = pltpu.SemaphoreType.DMA
    hbm = pl.BlockSpec(memory_space=pl.ANY)
    vmem = pl.BlockSpec(memory_space=pltpu.VMEM)
    return pl.pallas_call(
        functools.partial(body, nz, chunks),
        out_shape=(
            jax.ShapeDtypeStruct((count, LANES), F32),
            jax.ShapeDtypeStruct((8, count), F32),
            jax.ShapeDtypeStruct((32, width), F32),
            jax.ShapeDtypeStruct((32, width), F32),
            jax.ShapeDtypeStruct((32, width), F32),
        ),
        in_specs=[vmem, hbm, hbm, hbm, hbm, hbm],
        out_specs=(vmem,) * 5,
        scratch_shapes=[
            pltpu.VMEM((count, LANES), BF16),
            pltpu.VMEM((count, LANES), BF16),
            pltpu.VMEM((64, width), BF16),
            pltpu.VMEM((32, width), BF16),
            pltpu.VMEM((32, width), BF16),
            pltpu.VMEM((experts, 16, LANES), BF16),
            pltpu.VMEM((experts, 16, LANES), BF16),
            pltpu.VMEM((experts, LANES), F32),
            pltpu.VMEM((slots, width), BF16),
            pltpu.VMEM((slots, width), BF16),
            pltpu.VMEM((16, 64, LANES), BF16),
            pltpu.VMEM((16, 64, slots), BF16),
            pltpu.VMEM((16, 1, slots), F32),
            pltpu.VMEM((experts, 8, LANES), BF16),
            pltpu.VMEM((experts, 8, LANES), BF16),
            dma((5,)),
            dma((experts,)),
            dma((experts,)),
            dma((16,)),
            dma((16,)),
            dma((2, chunks, 8)),
            dma((2, chunks, 8)),
            dma((16,)),
            dma((16,)),
            dma((16,)),
            dma((16,)),
            dma((experts,)),
            dma((experts,)),
        ],
        compiler_params=pltpu.CompilerParams(collective_id=0, has_side_effects=True),
        name="experts",
    )(route, tokens, cotangent, wg, wu, wd)


def shards(
    nz,
    chunks,
    tokens,
    cotangent,
    group_weight,
    expert_weight,
    group_choice,
    local_choice,
    w_gate,
    w_up,
    w_down,
):
    ids = (group_choice[None, :] * EPG + local_choice.T).astype(F32)
    gate = (group_weight[None, :] * expert_weight.T).astype(BF16).astype(F32)
    zero = jnp.zeros((1, tokens.shape[0]), F32)
    route = jnp.concatenate([ids, gate, group_weight[None, :], expert_weight.T, zero], axis=0)
    token_grad, small, gate_grad, up_grad, down_grad = run(
        nz,
        chunks,
        route,
        tokens,
        cotangent,
        w_gate[0].T,
        w_up[0].T,
        w_down[0],
    )
    return (
        token_grad,
        small[2],
        small[0:2].T,
        gate_grad.T[None],
        up_grad.T[None],
        down_grad[None],
    )


def build(mesh, chunks):
    nz = mesh.shape["ep"] // 2
    split = Mesh(mesh.devices.reshape(nz, 2, 4, 4), ("z", "c", "y", "x"))
    ep, tp = ("z", "c"), ("y", "x")
    in_specs = (
        P(ep, None),
        P(ep, None),
        P(ep),
        P(ep, None),
        P(ep),
        P(ep, None),
        P(ep, None, tp),
        P(ep, None, tp),
        P(ep, tp, None),
    )
    out_specs = (
        P(ep, tp),
        P(ep),
        P(ep, None),
        P(ep, None, tp),
        P(ep, None, tp),
        P(ep, tp, None),
    )
    return jax.shard_map(
        functools.partial(shards, nz, chunks),
        mesh=split,
        in_specs=in_specs,
        out_specs=out_specs,
        check_vma=False,
    )


def solution(mesh):
    return build(mesh, 4)
```
